128 devices in a mesh: ep: 64 (over z, y, x), tp: 2 (over core).
Axes of the slice: x: 4, y: 4, z: 4, core: 2. Of those that a mesh axis runs over, the one named last changes fastest.
Arguments:
- tokens: bfloat16 [32768, 2048], P(('ep', 'tp')), may hold values from -6 to 6
- norm_gain: float32 [2048], replicated, may hold values from 0.1 to 1.9
- norm_bias: float32 [2048], replicated, may hold values from -3 to 3
- gate_weight: bfloat16 [64, 2048, 1024], P('ep', None, 'tp'), may hold values from -0.125 to 0.125
- up_weight: bfloat16 [64, 2048, 1024], P('ep', None, 'tp'), may hold values from -0.125 to 0.125
- down_weight: bfloat16 [64, 1024, 2048], P('ep', 'tp'), may hold values from -0.1875 to 0.1875
- expert_ids: int32 [32768, 2], P(('ep', 'tp')), may hold values from 0 to 63, all different within a row; in each aligned block of 256 rows (0 to 255, 256 to 511, ...) at most 16 rows name the same one
- route_weights: float32 [32768, 2], P(('ep', 'tp')), may hold values from 0.2 to 1
Outputs:
- mixed: bfloat16 [32768, 2048], P(('ep', 'tp'))
The draws below stay inside these ranges and needn't reach their ends.
Inputs may be any that keep to these rules, and one draw needn't show every extreme that they name: `expert_ids`: a token's 2 experts differ; in the tokens of one device (aligned blocks of 256 rows) no expert is named by more than 16 entries, a bound that some block reaches.
All inputs are finite; a program needn't handle non-finite values.
Results may differ from the reference program's by a relative error of at most 0.0071.
Values may be sent and summed in bfloat16 or wider, within the bound.
A program may use at most 128 MiB of HBM per device.

```python
import math
import jax
import jax.numpy as jnp
import numpy as np
from jax import lax

D = 2048
FFE = 1024
TOPK = 2
TOK_DEV = 256
EXPERTS = 64
CAP = 16
TOKENS = 32768


def block_scale(key, dims, cuts, least, high):
    def one(dim, shards_of):
        draws = jax.random.uniform(jax.random.fold_in(jax.random.fold_in(key, 6), dim), (shards_of,), jnp.float32, least / len(cuts), high / len(cuts))
        return jnp.repeat(jnp.exp(draws), dims[dim] // shards_of).reshape((-1,) + (1,) * (len(dims) - dim - 1))

    level = one(*cuts[0])
    for cut in cuts[1:]:
        level = level * one(*cut)
    return level


def assign_block(stream_key, own, number, rows, number_of, top, limit, skew):
    ranking = jax.random.permutation(stream_key, number_of)
    heavy_load, common = shares(number_of, rows * top, limit, skew, True), shares(number_of, rows * top, limit, skew, False)
    places = jnp.arange(number_of)

    def named(tallies, offset_by):
        used = int((tallies > 0).sum())
        fixed = max(1, used // 4)
        moved = fixed + (places - fixed + offset_by * (used - fixed)) % max(1, number_of - fixed)
        return jnp.zeros((number_of,), jnp.int32).at[ranking[jnp.where(places < fixed, places, moved)]].set(jnp.asarray(tallies, jnp.int32))

    tallies = jnp.where(number % 4 == 0, named(heavy_load, number // 4), named(common, number - number // 4 - 1))
    mixed = jax.random.permutation(jax.random.fold_in(own, 3), number_of)
    source_of, receiver = mixed[0:number_of // 2 * 2:2], mixed[1:number_of // 2 * 2:2]
    room = jnp.minimum(tallies[source_of] - 1, limit - tallies[receiver]) // 2
    room = jnp.where((source_of == ranking[0]) | (receiver == ranking[0]) | (tallies[receiver] == 0), 0, jnp.maximum(room, 0))
    moved = jax.random.randint(jax.random.fold_in(own, 4), (number_of // 2,), 0, 1 << 20) % (room + 1)
    tallies = tallies.at[source_of].add(-moved).at[receiver].add(moved)
    members = jnp.searchsorted(jnp.cumsum(tallies), jnp.arange(rows * top), side="right").astype(jnp.int32)
    grid = members.reshape(top, rows).T
    grid = grid[jax.random.permutation(jax.random.fold_in(own, 1), rows)]
    offset_by = jax.random.randint(jax.random.fold_in(own, 2), (rows, 1), 0, top)
    return jnp.take_along_axis(grid, (jnp.arange(top)[None, :] + offset_by) % top, axis=1)


def shares(number_of, total, bound, slope, full):
    loads = [(1 << 20) // math.isqrt(rank ** slope) + 1 for rank in range(1, number_of + 1)]
    largest = bound if full else min(bound, max(-(-total // number_of), total * loads[0] // sum(loads)))
    least = 1 if total - largest >= number_of - 1 else 0
    counts, rest = [largest] + [least] * (number_of - 1), total - largest - least * (number_of - 1)
    while rest > 0:
        candidates = [i for i in range(1, number_of) if counts[i] < largest] or [i for i in range(1, number_of) if counts[i] < bound]
        pool, left = sum([loads[i] for i in candidates]), rest
        for i in candidates:
            more = min(bound - counts[i], max(1, left * loads[i] // pool), rest)
            counts[i] = counts[i] + more
            rest = rest - more
    return np.array(counts)


def scatter_about(own_key, shape, width, bound, cuts=(), held_as=jnp.bfloat16):
    array = jax.random.normal(own_key, shape, jnp.float32) * width
    if len(cuts) > 0:
        array = block_scale(own_key, shape, cuts, -0.22, 0.18) * array
    return jnp.clip(array, min=-bound, max=bound).astype(held_as)


def setup_inputs(seed: int = 0) -> dict:
    seeds = jax.random.split(jax.random.key(seed), 9)
    tokens = scatter_about(seeds[0], (TOKENS, D), 1.0, 6.0, ((0, 128),))
    norm_gain = jnp.clip(1.0 + 0.18 * jax.random.normal(seeds[1], (D,), jnp.float32), 0.1, 1.9)
    norm_bias = scatter_about(seeds[2], (D,), 0.5, 3.0, (), jnp.float32)
    gate_weight = scatter_about(seeds[3], (EXPERTS, D, FFE), D ** -0.5, 0.125, ((0, 64), (2, 2)))
    up_weight = scatter_about(seeds[4], (EXPERTS, D, FFE), D ** -0.5, 0.125, ((0, 64), (2, 2)))
    down_weight = scatter_about(seeds[5], (EXPERTS, FFE, D), FFE ** -0.5, 0.1875, ((0, 64), (1, 2)))
    expert_ids_keys = jax.random.split(jax.random.fold_in(seeds[6], 1), TOKENS // TOK_DEV)
    expert_ids_turns = jax.random.permutation(jax.random.fold_in(seeds[6], 3), TOKENS // TOK_DEV)
    expert_ids = jax.vmap(lambda own, number: assign_block(jax.random.fold_in(seeds[6], 2), own, number, TOK_DEV, EXPERTS, TOPK, CAP, 2))(expert_ids_keys, expert_ids_turns).reshape((TOKENS, TOPK))
    route_weights = jnp.clip(0.2 + 0.8 * jax.random.uniform(seeds[7], (TOKENS, TOPK), jnp.float32) ** block_scale(seeds[7], (TOKENS, TOPK), ((0, 128),), -0.2, 0.2), 0.2, 1.0)
    return {"tokens": tokens, "norm_gain": norm_gain, "norm_bias": norm_bias, "gate_weight": gate_weight, "up_weight": up_weight, "down_weight": down_weight, "expert_ids": expert_ids, "route_weights": route_weights}


def expert_rows(rows, w_gate, w_up, w_down):
    gate = jnp.dot(rows, w_gate, preferred_element_type=jnp.float32)
    upper = jnp.dot(rows, w_up, preferred_element_type=jnp.float32)
    hidden = (jax.nn.silu(gate) * upper).astype(jnp.bfloat16)
    return jnp.dot(hidden, w_down, preferred_element_type=jnp.float32).astype(jnp.bfloat16)

def reference(tokens, norm_gain, norm_bias, gate_weight, up_weight, down_weight, expert_ids, route_weights):
    values = tokens.astype(jnp.float32)
    centre = values - lax.optimization_barrier(jnp.mean(values, axis=-1, keepdims=True))
    spread = lax.optimization_barrier(jnp.mean(centre * centre, axis=-1, keepdims=True))
    normed = (centre * lax.rsqrt(spread + 1e-05) * norm_gain + norm_bias).astype(jnp.bfloat16)
    sources = TOKENS // TOK_DEV
    blocks = expert_ids.reshape(sources, TOK_DEV * TOPK)
    onehot = (blocks[:, :, None] == jnp.arange(EXPERTS, dtype=jnp.int32)[None, None, :]).astype(jnp.int32)
    slot = lax.optimization_barrier(jnp.sum(jnp.cumsum(onehot, axis=1) * onehot, axis=-1)) - 1
    row_index = (jnp.arange(sources, dtype=jnp.int32)[:, None] * CAP + slot).reshape(-1).astype(jnp.int32)
    flat_ids = expert_ids.reshape(-1)
    token_rows = jnp.repeat(normed, TOPK, axis=0)
    buffer_rows = sources * CAP

    def one_expert(expert, total):
        chosen = flat_ids == expert
        index = jnp.where(chosen, row_index, buffer_rows).astype(jnp.int32)
        buffer = jnp.zeros((buffer_rows, D), jnp.bfloat16).at[index].set(token_rows, mode='drop')
        result = expert_rows(buffer, gate_weight[expert], up_weight[expert], down_weight[expert])
        picked = result[jnp.minimum(index, buffer_rows - 1)]
        picked = jnp.where(chosen[:, None], picked.astype(jnp.float32), 0.0).reshape(TOKENS, TOPK, D)
        return total + lax.optimization_barrier(jnp.sum(picked * route_weights[:, :, None], axis=1))
    total = lax.fori_loop(0, EXPERTS, one_expert, jnp.zeros((TOKENS, D), jnp.float32))
    return total.astype(jnp.bfloat16)
```

```python
import jax
import jax.numpy as jnp
from jax import lax
from jax.experimental import pallas as pl
from jax.experimental.pallas import tpu as pltpu
from jax.sharding import PartitionSpec as P

MESH = pl.DeviceIdType.MESH
CAP = 16
GROUPS = 4
PER = 16
F32 = jnp.float32
BF16 = jnp.bfloat16


def chip_at(place, ep, sign):
    k, j = place >> 4, place & 15
    dz, dy = j >> 2, j & 3
    dx = (k - dz - dy) & 3
    z, y, x = ep >> 4, (ep >> 2) & 3, ep & 3
    return (((z + sign * dz) & 3) << 4) | (((y + sign * dy) & 3) << 2) | ((x + sign * dx) & 3)


def kernel(
    tok, gain, bias, ids, rw, wg, wu, wd, out,
    normed, pick, send, recv, res, ret, vg, vu, vd, hid, whi, wlo, acc,
    local_sem, wsend_sem, wrecv_sem, dsend, drecv, rsend, rrecv,
):
    ep, tp = lax.axis_index("ep"), lax.axis_index("tp")
    rows, width = tok.shape
    half = wg.shape[1]
    experts = lax.axis_size("ep")

    barrier = pltpu.get_barrier_semaphore()

    def greet(i, carry):
        pl.semaphore_signal(barrier, inc=1, device_id={"ep": (ep + i) % experts, "tp": tp}, device_id_type=MESH)
        return carry

    lax.fori_loop(1, experts, greet, 0)
    pl.semaphore_signal(barrier, inc=1, device_id={"ep": ep, "tp": 1 - tp}, device_id_type=MESH)

    mine = pl.ds(pl.multiple_of(tp * half, half), half)
    pairs = ((wg, vg.at[tp]), (wu, vu.at[tp]), (wd, vd.at[mine]))
    local = [pltpu.make_async_copy(a, b, local_sem.at[n]) for n, (a, b) in enumerate(pairs)]
    shared = [
        pltpu.make_async_remote_copy(
            src_ref=a, dst_ref=b, send_sem=wsend_sem.at[n], recv_sem=wrecv_sem.at[n],
            device_id={"ep": ep, "tp": 1 - tp}, device_id_type=MESH,
        )
        for n, (a, b) in enumerate(pairs)
    ]
    for copy in local:
        copy.start()

    step = 32

    def norm(n, carry):
        at = pl.ds(pl.multiple_of(n * step, step), step)
        values = tok[at, :].astype(F32)
        centre = values - jnp.mean(values, axis=-1, keepdims=True)
        spread = jnp.mean(centre * centre, axis=-1, keepdims=True)
        normed[at, :] = (centre * lax.rsqrt(spread + 1e-05) * gain[...] + bias[...]).astype(BF16)
        return carry

    lax.fori_loop(0, rows // step, norm, 0)

    lanes = lax.broadcasted_iota(jnp.int32, (rows, 128), 1)
    first, second = ids[:, 0:1] == lanes, ids[:, 1:2] == lanes
    named = jnp.where(first | second, 1.0, 0.0)
    earlier = lax.broadcasted_iota(jnp.int32, (rows, rows), 1) < lax.broadcasted_iota(jnp.int32, (rows, rows), 0)
    count = jnp.dot(jnp.where(earlier, 1.0, 0.0).astype(BF16), named.astype(BF16), preferred_element_type=F32)
    slot = jnp.where(named > 0.0, count, -1.0)

    total = experts * CAP
    place = lax.broadcasted_iota(jnp.int32, (total, 128), 0)
    chip = chip_at(place >> 4, ep, 1)
    spread_rows = jnp.where(lax.broadcasted_iota(jnp.int32, (total, 128), 1) == chip, 1.0, 0.0).astype(BF16)
    slot_of = jnp.dot(spread_rows, slot.T.astype(BF16), preferred_element_type=F32)
    wanted = (lax.broadcasted_iota(jnp.int32, (total, rows), 0) & 15).astype(F32)
    pick[...] = jnp.where(slot_of == wanted, 1.0, 0.0).astype(BF16)

    pl.semaphore_wait(barrier, experts)
    for copy in shared:
        copy.start()

    def dispatch_copy(i):
        return pltpu.make_async_remote_copy(
            src_ref=send.at[i], dst_ref=recv.at[i], send_sem=dsend.at[i], recv_sem=drecv.at[i],
            device_id={"ep": chip_at(i, ep, 1), "tp": tp}, device_id_type=MESH,
        )

    def return_copy(i):
        return pltpu.make_async_remote_copy(
            src_ref=res.at[i], dst_ref=ret.at[i], send_sem=rsend.at[i], recv_sem=rrecv.at[i],
            device_id={"ep": chip_at(i, ep, -1), "tp": tp}, device_id_type=MESH,
        )

    def each(low, high, action):
        def run(i, carry):
            action(i)
            return carry

        lax.fori_loop(low, high, run, 0)

    def fill(k):
        chosen = pick[pl.ds(pl.multiple_of(k * PER * CAP, PER * CAP), PER * CAP), :]
        for c in range(0, width, 512):
            piece = jnp.dot(chosen, normed[:, c : c + 512], preferred_element_type=F32).astype(BF16)
            send[pl.ds(k * PER, PER), :, c : c + 512] = piece.reshape(PER, CAP, 512)

    fill(0)
    recv[0] = send[0]

    def push(k, carry):
        fill(k)
        each(jnp.maximum((k - 1) * PER, 1), k * PER, lambda i: dispatch_copy(i).start())
        return carry

    lax.fori_loop(1, GROUPS, push, 0)

    place = lax.broadcasted_iota(jnp.int32, (128, total), 1)
    chip = chip_at(place >> 4, ep, 1)
    spread_cols = jnp.where(lax.broadcasted_iota(jnp.int32, (128, total), 0) == chip, 1.0, 0.0).astype(BF16)
    each((GROUPS - 1) * PER, GROUPS * PER, lambda i: dispatch_copy(i).start())
    weight = jnp.where(first, rw[:, 0:1], 0.0) + jnp.where(second, rw[:, 1:2], 0.0)
    high = weight.astype(BF16)
    low = (weight - high.astype(F32)).astype(BF16)
    here = jnp.dot(slot.astype(BF16), spread_cols, preferred_element_type=F32) == (
        lax.broadcasted_iota(jnp.int32, (rows, total), 1) & 15
    ).astype(F32)
    whi[...] = jnp.where(here, jnp.dot(high, spread_cols, preferred_element_type=F32), 0.0).astype(BF16)
    wlo[...] = jnp.where(here, jnp.dot(low, spread_cols, preferred_element_type=F32), 0.0).astype(BF16)

    for copy in local:
        copy.wait()
    for copy in shared:
        copy.wait_recv()

    def expert(k, carry):
        each(jnp.maximum(k * PER, 1), (k + 1) * PER, lambda i: dispatch_copy(i).wait_recv())
        x = recv[pl.ds(k * PER, PER)].reshape(PER * CAP, width)
        for t in range(2):
            for c in range(0, half, 256):
                gate = jnp.dot(x, vg[t, :, c : c + 256], preferred_element_type=F32)
                upper = jnp.dot(x, vu[t, :, c : c + 256], preferred_element_type=F32)
                hid[:, t * half + c : t * half + c + 256] = (gate / (1.0 + jnp.exp(-gate)) * upper).astype(BF16)
        for c in range(0, width, 256):
            piece = jnp.dot(hid[...], vd[:, c : c + 256], preferred_element_type=F32).astype(BF16)
            res[pl.ds(k * PER, PER), :, c : c + 256] = piece.reshape(PER, CAP, 256)
        each(jnp.maximum(k * PER, 1), (k + 1) * PER, lambda i: return_copy(i).start())
        return carry

    lax.fori_loop(0, GROUPS, expert, 0)
    ret[0] = res[0]

    acc[...] = jnp.zeros_like(acc)

    def combine(k, carry):
        each(jnp.maximum(k * PER, 1), (k + 1) * PER, lambda i: return_copy(i).wait_recv())
        at = pl.ds(pl.multiple_of(k * PER * CAP, PER * CAP), PER * CAP)
        for c in range(0, width, 512):
            y = ret[pl.ds(k * PER, PER), :, c : c + 512].reshape(PER * CAP, 512)
            acc[:, c : c + 512] += jnp.dot(whi[:, at], y, preferred_element_type=F32) + jnp.dot(
                wlo[:, at], y, preferred_element_type=F32
            )
        return carry

    lax.fori_loop(0, GROUPS, combine, 0)
    out[...] = acc[...].astype(BF16)

    for copy in shared:
        copy.wait_send()
    each(1, GROUPS * PER, lambda i: dispatch_copy(i).wait_send())
    each(1, GROUPS * PER, lambda i: return_copy(i).wait_send())


def body(tokens, norm_gain, norm_bias, gate_weight, up_weight, down_weight, expert_ids, route_weights):
    rows, width = tokens.shape
    half = gate_weight.shape[2]
    experts = lax.axis_size("ep")
    total = experts * CAP
    vmem = pl.BlockSpec(memory_space=pltpu.VMEM)
    hbm = pl.BlockSpec(memory_space=pltpu.HBM)
    buffers = pltpu.VMEM((experts, CAP, width), BF16)
    copies = pltpu.SemaphoreType.DMA((experts,))
    three = pltpu.SemaphoreType.DMA((3,))
    return pl.pallas_call(
        kernel,
        name="experts",
        out_shape=jax.ShapeDtypeStruct((rows, width), BF16),
        in_specs=[vmem] * 5 + [hbm] * 3,
        out_specs=vmem,
        scratch_shapes=[
            pltpu.VMEM((rows, width), BF16),
            pltpu.VMEM((total, rows), BF16),
            buffers, buffers, buffers, buffers,
            pltpu.VMEM((2, width, half), BF16),
            pltpu.VMEM((2, width, half), BF16),
            pltpu.VMEM((2 * half, width), BF16),
            pltpu.VMEM((PER * CAP, 2 * half), BF16),
            pltpu.VMEM((rows, total), BF16),
            pltpu.VMEM((rows, total), BF16),
            pltpu.VMEM((rows, width), F32),
            three, three, three, copies, copies, copies, copies,
        ],
        compiler_params=pltpu.CompilerParams(
            collective_id=0, has_side_effects=True, vmem_limit_bytes=60 * 1024 * 1024
        ),
    )(
        tokens, norm_gain.reshape(1, width), norm_bias.reshape(1, width), expert_ids, route_weights,
        gate_weight[0], up_weight[0], down_weight[0],
    )


def solution(mesh):
    placed = (
        P(("ep", "tp"), None),
        P(),
        P(),
        P("ep", None, "tp"),
        P("ep", None, "tp"),
        P("ep", "tp", None),
        P(("ep", "tp"), None),
        P(("ep", "tp"), None),
    )
    return jax.shard_map(body, mesh=mesh, in_specs=placed, out_specs=P(("ep", "tp"), None), check_vma=False)
```

```python
import jax
import jax.numpy as jnp
from jax import lax
from jax.experimental import pallas as pl
from jax.experimental.pallas import tpu as pltpu
from jax.sharding import PartitionSpec as P

MESH = pl.DeviceIdType.MESH
CAP = 16
GROUPS = 8
PER = 64 // GROUPS
F32 = jnp.float32
BF16 = jnp.bfloat16
PLACES = (
    0o000, 0o332, 0o221, 0o113, 0o211, 0o313, 0o131, 0o033,
    0o321, 0o213, 0o331, 0o123, 0o311, 0o133, 0o001, 0o103,
    0o230, 0o300, 0o112, 0o121, 0o323, 0o032, 0o011, 0o203,
    0o010, 0o320, 0o122, 0o101, 0o223, 0o002, 0o301, 0o233,
    0o120, 0o020, 0o200, 0o322, 0o201, 0o003, 0o132, 0o312,
    0o110, 0o330, 0o222, 0o111, 0o333, 0o102, 0o021, 0o303,
    0o210, 0o220, 0o100, 0o232, 0o031, 0o013, 0o022, 0o302,
    0o030, 0o310, 0o130, 0o212, 0o231, 0o023, 0o202, 0o012,
)


def kernel(
    tok, small, wg, wu, wd, out,
    rows_in,
    normed, spread, pick, send, recv, res, ret, vg, vu, vd, hid, whi, wlo, acc,
    in_sem, local_sem, wsend_sem, wrecv_sem, dsend, drecv, rsend, rrecv,
):
    ep, tp = lax.axis_index("ep"), lax.axis_index("tp")
    rows, width = tok.shape
    half = wg.shape[1]
    experts = lax.axis_size("ep")
    z, y, x = ep >> 4, (ep >> 2) & 3, ep & 3
    ahead = [[((at + d) & 3) << shift for d in range(4)] for at, shift in ((z, 4), (y, 2), (x, 0))]
    behind = [[((at - d) & 3) << shift for d in range(4)] for at, shift in ((z, 4), (y, 2), (x, 0))]

    def chip_at(i, steps):
        place = PLACES[i]
        return steps[0][place >> 6] | steps[1][(place >> 3) & 7] | steps[2][place & 7]

    block = rows // 4
    token_rows = [
        pltpu.make_async_copy(tok.at[pl.ds(n * block, block)], rows_in.at[pl.ds(n * block, block)], in_sem.at[n])
        for n in range(4)
    ]
    for copy in token_rows:
        copy.start()

    barrier = pltpu.get_barrier_semaphore()

    def greet(i, carry):
        pl.semaphore_signal(barrier, inc=1, device_id={"ep": (ep + i) & (experts - 1), "tp": tp}, device_id_type=MESH)
        return carry

    pl.semaphore_signal(barrier, inc=1, device_id={"ep": ep, "tp": 1 - tp}, device_id_type=MESH)
    with jax.named_scope("s_greet"):
        lax.fori_loop(1, experts, greet, 0)

    mine = pl.ds(pl.multiple_of(tp * half, half), half)
    pairs = ((wg, vg.at[tp]), (wu, vu.at[tp]), (wd, vd.at[mine]))
    local = [pltpu.make_async_copy(a, b, local_sem.at[n]) for n, (a, b) in enumerate(pairs)]
    shared = [
        pltpu.make_async_remote_copy(
            src_ref=a, dst_ref=b, send_sem=wsend_sem.at[n], recv_sem=wrecv_sem.at[n],
            device_id={"ep": ep, "tp": 1 - tp}, device_id_type=MESH,
        )
        for n, (a, b) in enumerate(pairs)
    ]

    with jax.named_scope("s_route"):
        later = lax.broadcasted_iota(jnp.int32, (rows, rows), 0) < lax.broadcasted_iota(jnp.int32, (rows, rows), 1)
        later = jnp.where(later, 1.0, 0.0).astype(BF16)
        total = experts * CAP
        lanes = lax.broadcasted_iota(jnp.int32, (CAP, 128), 1)
        for i in range(experts):
            spread[i * CAP : (i + 1) * CAP, :] = jnp.where(lanes == chip_at(i, ahead), 1.0, 0.0).astype(BF16)
        expert_rows = lax.broadcasted_iota(jnp.int32, (128, rows), 0).astype(F32)
        first, second = small[0:1, width : width + rows] == expert_rows, small[1:2, width : width + rows] == expert_rows
        named = first | second
        count = jnp.dot(jnp.where(named, 1.0, 0.0).astype(BF16), later, preferred_element_type=F32)
        slot = jnp.where(named, count, -1.0)
        slot_of = jnp.dot(spread[...], slot.astype(BF16), preferred_element_type=F32)
        wanted = (lax.broadcasted_iota(jnp.int32, (total, rows), 0) & 15).astype(F32)
        pick[...] = jnp.where(slot_of == wanted, 1.0, 0.0).astype(BF16)

    with jax.named_scope("s_ln"):
        step = 32

        def norm(n, carry):
            at = pl.ds(pl.multiple_of(n * step, step), step)
            values = rows_in[at, :].astype(F32)
            centre = values - jnp.mean(values, axis=-1, keepdims=True)
            spread = jnp.mean(centre * centre, axis=-1, keepdims=True)
            normed[at, :] = (centre * lax.rsqrt(spread + 1e-05) * small[0:1, 0:width] + small[1:2, 0:width]).astype(BF16)
            return carry

        for copy in token_rows:
            copy.wait()
        lax.fori_loop(0, rows // step, norm, 0)

    def dispatch_copy(i):
        return pltpu.make_async_remote_copy(
            src_ref=send.at[i], dst_ref=recv.at[i], send_sem=dsend.at[i], recv_sem=drecv.at[i],
            device_id={"ep": chip_at(i, ahead), "tp": tp}, device_id_type=MESH,
        )

    def return_copy(i):
        return pltpu.make_async_remote_copy(
            src_ref=res.at[i], dst_ref=ret.at[i], send_sem=rsend.at[i], recv_sem=rrecv.at[i],
            device_id={"ep": chip_at(i, behind), "tp": tp}, device_id_type=MESH,
        )

    def members(k, action):
        for g in range(GROUPS):

            @pl.when(k == g)
            def _():
                for i in range(max(g * PER, 1), (g + 1) * PER):
                    action(i)

    def fill(k):
        chosen = pick[pl.ds(pl.multiple_of(k * PER * CAP, PER * CAP), PER * CAP), :]
        for c in range(0, width, 512):
            piece = jnp.dot(chosen, normed[:, c : c + 512], preferred_element_type=F32).astype(BF16)
            send[pl.ds(k * PER, PER), :, c : c + 512] = piece.reshape(PER, CAP, 512)

    fill(0)
    with jax.named_scope("s_bar"):
        pl.semaphore_wait(barrier, experts)
    for i in range(1, PER):
        dispatch_copy(i).start()
    for copy in shared:
        copy.start()
    for copy in local:
        copy.start()
    recv[0] = send[0]

    with jax.named_scope("s_push"):
        for k in range(1, GROUPS):
            fill(k)
            for i in range(k * PER, (k + 1) * PER):
                dispatch_copy(i).start()

    def to_rows(v):
        return lax.dot_general(v, spread[...], (((1,), (1,)), ((), ())), preferred_element_type=F32)

    weight = (jnp.where(first, small[0:1, width + rows : width + 2 * rows], 0.0) + jnp.where(second, small[1:2, width + rows : width + 2 * rows], 0.0)).T
    high = weight.astype(BF16)
    low = (weight - high.astype(F32)).astype(BF16)
    here = to_rows(slot.T.astype(BF16)) == (
        lax.broadcasted_iota(jnp.int32, (rows, total), 1) & 15
    ).astype(F32)
    whi[...] = jnp.where(here, to_rows(high), 0.0).astype(BF16)
    wlo[...] = jnp.where(here, to_rows(low), 0.0).astype(BF16)
    acc[...] = jnp.zeros_like(acc)

    with jax.named_scope("s_wwait"):
        for copy in local:
            copy.wait()
        for copy in shared:
            copy.wait_recv()

    def expert(k, carry):
        with jax.named_scope("s_dwait"):
            members(k, lambda i: dispatch_copy(i).wait_recv())
        x = recv[pl.ds(k * PER, PER)].reshape(PER * CAP, width)
        for t in range(2):
            for c in range(0, half, 256):
                gate = jnp.dot(x, vg[t, :, c : c + 256], preferred_element_type=F32)
                upper = jnp.dot(x, vu[t, :, c : c + 256], preferred_element_type=F32)
                hid[:, t * half + c : t * half + c + 256] = (gate / (1.0 + jnp.exp(-gate)) * upper).astype(BF16)
        for c in range(0, width, 256):
            piece = jnp.dot(hid[...], vd[:, c : c + 256], preferred_element_type=F32).astype(BF16)
            res[pl.ds(k * PER, PER), :, c : c + 256] = piece.reshape(PER, CAP, 256)
        with jax.named_scope("s_rsend"):
            members(k, lambda i: return_copy(i).start())
        return carry

    lax.fori_loop(0, GROUPS, expert, 0)
    ret[0] = res[0]

    def combine(k, carry):
        with jax.named_scope("s_rwait"):
            members(k, lambda i: return_copy(i).wait_recv())
        at = pl.ds(pl.multiple_of(k * PER * CAP, PER * CAP), PER * CAP)
        for c in range(0, width, 512):
            y = ret[pl.ds(k * PER, PER), :, c : c + 512].reshape(PER * CAP, 512)
            acc[:, c : c + 512] += jnp.dot(whi[:, at], y, preferred_element_type=F32) + jnp.dot(
                wlo[:, at], y, preferred_element_type=F32
            )
        return carry

    lax.fori_loop(0, GROUPS, combine, 0)
    with jax.named_scope("s_out"):
        out[...] = acc[...].astype(BF16)

    with jax.named_scope("s_end"):
        for copy in shared:
            copy.wait_send()
        for i in range(1, experts):
            dispatch_copy(i).wait_send()
            return_copy(i).wait_send()


def body(tokens, norm_gain, norm_bias, gate_weight, up_weight, down_weight, expert_ids, route_weights):
    rows, width = tokens.shape
    half = gate_weight.shape[2]
    experts = lax.axis_size("ep")
    total = experts * CAP
    small = jnp.concatenate((jnp.stack((norm_gain, norm_bias)), expert_ids.T.astype(F32), route_weights.T), axis=1)
    hbm = pl.BlockSpec(memory_space=pltpu.HBM)
    buffers = pltpu.VMEM((experts, CAP, width), BF16)
    copies = pltpu.SemaphoreType.DMA((experts,))
    three = pltpu.SemaphoreType.DMA((3,))
    return pl.pallas_call(
        kernel,
        name="experts",
        out_shape=jax.ShapeDtypeStruct((rows, width), BF16),
        in_specs=[hbm, pl.BlockSpec(memory_space=pltpu.VMEM), hbm, hbm, hbm],
        out_specs=pl.BlockSpec(memory_space=pltpu.VMEM),
        scratch_shapes=[
            pltpu.VMEM((rows, width), BF16),
            pltpu.VMEM((rows, width), BF16),
            pltpu.VMEM((total, 128), BF16),
            pltpu.VMEM((total, rows), BF16),
            buffers, buffers, buffers, buffers,
            pltpu.VMEM((2, width, half), BF16),
            pltpu.VMEM((2, width, half), BF16),
            pltpu.VMEM((2 * half, width), BF16),
            pltpu.VMEM((PER * CAP, 2 * half), BF16),
            pltpu.VMEM((rows, total), BF16),
            pltpu.VMEM((rows, total), BF16),
            pltpu.VMEM((rows, width), F32),
            pltpu.SemaphoreType.DMA((4,)),
            three, three, three, copies, copies, copies, copies,
        ],
        compiler_params=pltpu.CompilerParams(
            collective_id=0, has_side_effects=True, vmem_limit_bytes=52 * 1024 * 1024
        ),
    )(
        tokens, small,
        gate_weight[0], up_weight[0], down_weight[0],
    )


def solution(mesh):
    placed = (
        P(("ep", "tp"), None),
        P(),
        P(),
        P("ep", None, "tp"),
        P("ep", None, "tp"),
        P("ep", "tp", None),
        P(("ep", "tp"), None),
        P(("ep", "tp"), None),
    )
    return jax.shard_map(body, mesh=mesh, in_specs=placed, out_specs=P(("ep", "tp"), None), check_vma=False)
```

```python
import jax
import jax.numpy as jnp
from jax import lax
from jax.experimental import pallas as pl
from jax.experimental.pallas import tpu as pltpu
from jax.sharding import PartitionSpec as P

MESH = pl.DeviceIdType.MESH
CAP = 16
GROUPS = 8
PER = 64 // GROUPS
F32 = jnp.float32
BF16 = jnp.bfloat16
PLACES = (
    0o000, 0o121, 0o202, 0o323, 0o112, 0o233, 0o310, 0o031,
    0o220, 0o301, 0o022, 0o103, 0o332, 0o013, 0o130, 0o211,
    0o001, 0o122, 0o203, 0o320, 0o113, 0o230, 0o311, 0o032,
    0o221, 0o302, 0o023, 0o100, 0o333, 0o010, 0o131, 0o212,
    0o002, 0o123, 0o200, 0o321, 0o110, 0o231, 0o312, 0o033,
    0o222, 0o303, 0o020, 0o101, 0o330, 0o011, 0o132, 0o213,
    0o003, 0o120, 0o201, 0o322, 0o111, 0o232, 0o313, 0o030,
    0o223, 0o300, 0o021, 0o102, 0o331, 0o012, 0o133, 0o210,
)


def kernel(
    tok, gain, bias, ids, rw, wg, wu, wd, out,
    rows_in, gain_in, bias_in, ids_in, rw_in,
    normed, spread, pick, send, recv, res, ret, vg, vu, vd, hid, whi, wlo, acc,
    in_sem, local_sem, wsend_sem, wrecv_sem, dsend, drecv, rsend, rrecv,
):
    ep, tp = lax.axis_index("ep"), lax.axis_index("tp")
    rows, width = tok.shape
    half = wg.shape[1]
    experts = lax.axis_size("ep")
    z, y, x = ep >> 4, (ep >> 2) & 3, ep & 3
    ahead = [[((at + d) & 3) << shift for d in range(4)] for at, shift in ((z, 4), (y, 2), (x, 0))]
    behind = [[((at - d) & 3) << shift for d in range(4)] for at, shift in ((z, 4), (y, 2), (x, 0))]

    def chip_at(i, steps):
        place = PLACES[i]
        return steps[0][place >> 6] | steps[1][(place >> 3) & 7] | steps[2][place & 7]

    block = rows // 4
    inputs = [
        pltpu.make_async_copy(a, b, in_sem.at[n])
        for n, (a, b) in enumerate(((ids, ids_in), (rw, rw_in), (gain, gain_in), (bias, bias_in)))
    ]
    token_rows = [
        pltpu.make_async_copy(tok.at[pl.ds(n * block, block)], rows_in.at[pl.ds(n * block, block)], in_sem.at[4 + n])
        for n in range(4)
    ]
    for copy in inputs + token_rows:
        copy.start()

    barrier = pltpu.get_barrier_semaphore()

    def greet(i, carry):
        pl.semaphore_signal(barrier, inc=1, device_id={"ep": (ep + i) & (experts - 1), "tp": tp}, device_id_type=MESH)
        return carry

    pl.semaphore_signal(barrier, inc=1, device_id={"ep": ep, "tp": 1 - tp}, device_id_type=MESH)
    with jax.named_scope("s_greet"):
        lax.fori_loop(1, experts, greet, 0)

    mine = pl.ds(pl.multiple_of(tp * half, half), half)
    pairs = ((wg, vg.at[tp]), (wu, vu.at[tp]), (wd, vd.at[mine]))
    local = [pltpu.make_async_copy(a, b, local_sem.at[n]) for n, (a, b) in enumerate(pairs)]
    shared = [
        pltpu.make_async_remote_copy(
            src_ref=a, dst_ref=b, send_sem=wsend_sem.at[n], recv_sem=wrecv_sem.at[n],
            device_id={"ep": ep, "tp": 1 - tp}, device_id_type=MESH,
        )
        for n, (a, b) in enumerate(pairs)
    ]

    with jax.named_scope("s_route"):
        later = lax.broadcasted_iota(jnp.int32, (rows, rows), 0) < lax.broadcasted_iota(jnp.int32, (rows, rows), 1)
        later = jnp.where(later, 1.0, 0.0).astype(BF16)
        total = experts * CAP
        lanes = lax.broadcasted_iota(jnp.int32, (CAP, 128), 1)
        for i in range(experts):
            spread[i * CAP : (i + 1) * CAP, :] = jnp.where(lanes == chip_at(i, ahead), 1.0, 0.0).astype(BF16)
        for copy in inputs:
            copy.wait()
        expert_rows = lax.broadcasted_iota(jnp.int32, (128, rows), 0)
        first, second = ids_in[0:1, :] == expert_rows, ids_in[1:2, :] == expert_rows
        named = first | second
        count = jnp.dot(jnp.where(named, 1.0, 0.0).astype(BF16), later, preferred_element_type=F32)
        slot = jnp.where(named, count, -1.0)
        slot_of = jnp.dot(spread[...], slot.astype(BF16), preferred_element_type=F32)
        wanted = (lax.broadcasted_iota(jnp.int32, (total, rows), 0) & 15).astype(F32)
        pick[...] = jnp.where(slot_of == wanted, 1.0, 0.0).astype(BF16)

    with jax.named_scope("s_ln"):
        step = 32

        def norm(n, carry):
            at = pl.ds(pl.multiple_of(n * step, step), step)
            values = rows_in[at, :].astype(F32)
            centre = values - jnp.mean(values, axis=-1, keepdims=True)
            spread = jnp.mean(centre * centre, axis=-1, keepdims=True)
            normed[at, :] = (centre * lax.rsqrt(spread + 1e-05) * gain_in[...] + bias_in[...]).astype(BF16)
            return carry

        for copy in token_rows:
            copy.wait()
        lax.fori_loop(0, rows // step, norm, 0)

    def dispatch_copy(i):
        return pltpu.make_async_remote_copy(
            src_ref=send.at[i], dst_ref=recv.at[i], send_sem=dsend.at[i], recv_sem=drecv.at[i],
            device_id={"ep": chip_at(i, ahead), "tp": tp}, device_id_type=MESH,
        )

    def return_copy(i):
        return pltpu.make_async_remote_copy(
            src_ref=res.at[i], dst_ref=ret.at[i], send_sem=rsend.at[i], recv_sem=rrecv.at[i],
            device_id={"ep": chip_at(i, behind), "tp": tp}, device_id_type=MESH,
        )

    def members(k, action):
        for g in range(GROUPS):

            @pl.when(k == g)
            def _():
                for i in range(max(g * PER, 1), (g + 1) * PER):
                    action(i)

    def fill(k):
        chosen = pick[pl.ds(pl.multiple_of(k * PER * CAP, PER * CAP), PER * CAP), :]
        for c in range(0, width, 512):
            piece = jnp.dot(chosen, normed[:, c : c + 512], preferred_element_type=F32).astype(BF16)
            send[pl.ds(k * PER, PER), :, c : c + 512] = piece.reshape(PER, CAP, 512)

    fill(0)
    with jax.named_scope("s_bar"):
        pl.semaphore_wait(barrier, experts)
    for i in range(1, PER):
        dispatch_copy(i).start()
    for copy in shared:
        copy.start()
    for copy in local:
        copy.start()
    recv[0] = send[0]

    with jax.named_scope("s_push"):
        for k in range(1, GROUPS):
            fill(k)
            for i in range(k * PER, (k + 1) * PER):
                dispatch_copy(i).start()

    def to_rows(v):
        return lax.dot_general(v, spread[...], (((1,), (1,)), ((), ())), preferred_element_type=F32)

    weight = (jnp.where(first, rw_in[0:1, :], 0.0) + jnp.where(second, rw_in[1:2, :], 0.0)).T
    high = weight.astype(BF16)
    low = (weight - high.astype(F32)).astype(BF16)
    here = to_rows(slot.T.astype(BF16)) == (
        lax.broadcasted_iota(jnp.int32, (rows, total), 1) & 15
    ).astype(F32)
    whi[...] = jnp.where(here, to_rows(high), 0.0).astype(BF16)
    wlo[...] = jnp.where(here, to_rows(low), 0.0).astype(BF16)
    acc[...] = jnp.zeros_like(acc)

    with jax.named_scope("s_wwait"):
        for copy in local:
            copy.wait()
        for copy in shared:
            copy.wait_recv()

    def expert(k, carry):
        with jax.named_scope("s_dwait"):
            members(k, lambda i: dispatch_copy(i).wait_recv())
        x = recv[pl.ds(k * PER, PER)].reshape(PER * CAP, width)
        for t in range(2):
            for c in range(0, half, 256):
                gate = jnp.dot(x, vg[t, :, c : c + 256], preferred_element_type=F32)
                upper = jnp.dot(x, vu[t, :, c : c + 256], preferred_element_type=F32)
                hid[:, t * half + c : t * half + c + 256] = (gate / (1.0 + jnp.exp(-gate)) * upper).astype(BF16)
        for c in range(0, width, 256):
            piece = jnp.dot(hid[...], vd[:, c : c + 256], preferred_element_type=F32).astype(BF16)
            res[pl.ds(k * PER, PER), :, c : c + 256] = piece.reshape(PER, CAP, 256)
        with jax.named_scope("s_rsend"):
            members(k, lambda i: return_copy(i).start())
        return carry

    lax.fori_loop(0, GROUPS, expert, 0)
    ret[0] = res[0]

    def combine(k, carry):
        with jax.named_scope("s_rwait"):
            members(k, lambda i: return_copy(i).wait_recv())
        at = pl.ds(pl.multiple_of(k * PER * CAP, PER * CAP), PER * CAP)
        for c in range(0, width, 512):
            y = ret[pl.ds(k * PER, PER), :, c : c + 512].reshape(PER * CAP, 512)
            acc[:, c : c + 512] += jnp.dot(whi[:, at], y, preferred_element_type=F32) + jnp.dot(
                wlo[:, at], y, preferred_element_type=F32
            )
        return carry

    lax.fori_loop(0, GROUPS, combine, 0)
    with jax.named_scope("s_out"):
        out[...] = acc[...].astype(BF16)

    with jax.named_scope("s_end"):
        for copy in shared:
            copy.wait_send()
        for i in range(1, experts):
            dispatch_copy(i).wait_send()
            return_copy(i).wait_send()


def body(tokens, norm_gain, norm_bias, gate_weight, up_weight, down_weight, expert_ids, route_weights):
    rows, width = tokens.shape
    half = gate_weight.shape[2]
    experts = lax.axis_size("ep")
    total = experts * CAP
    hbm = pl.BlockSpec(memory_space=pltpu.HBM)
    buffers = pltpu.VMEM((experts, CAP, width), BF16)
    copies = pltpu.SemaphoreType.DMA((experts,))
    three = pltpu.SemaphoreType.DMA((3,))
    return pl.pallas_call(
        kernel,
        name="experts",
        out_shape=jax.ShapeDtypeStruct((rows, width), BF16),
        in_specs=[hbm] * 8,
        out_specs=pl.BlockSpec(memory_space=pltpu.VMEM),
        scratch_shapes=[
            pltpu.VMEM((rows, width), BF16),
            pltpu.VMEM((1, width), F32),
            pltpu.VMEM((1, width), F32),
            pltpu.VMEM((2, rows), jnp.int32),
            pltpu.VMEM((2, rows), F32),
            pltpu.VMEM((rows, width), BF16),
            pltpu.VMEM((total, 128), BF16),
            pltpu.VMEM((total, rows), BF16),
            buffers, buffers, buffers, buffers,
            pltpu.VMEM((2, width, half), BF16),
            pltpu.VMEM((2, width, half), BF16),
            pltpu.VMEM((2 * half, width), BF16),
            pltpu.VMEM((PER * CAP, 2 * half), BF16),
            pltpu.VMEM((rows, total), BF16),
            pltpu.VMEM((rows, total), BF16),
            pltpu.VMEM((rows, width), F32),
            pltpu.SemaphoreType.DMA((8,)),
            three, three, three, copies, copies, copies, copies,
        ],
        compiler_params=pltpu.CompilerParams(
            collective_id=0, has_side_effects=True, vmem_limit_bytes=52 * 1024 * 1024
        ),
    )(*(
        pltpu.with_memory_space_constraint(array, pltpu.HBM)
        for array in (
            tokens, norm_gain.reshape(1, width), norm_bias.reshape(1, width), expert_ids.T, route_weights.T,
            gate_weight[0], up_weight[0], down_weight[0],
        )
    ))


def solution(mesh):
    placed = (
        P(("ep", "tp"), None),
        P(),
        P(),
        P("ep", None, "tp"),
        P("ep", None, "tp"),
        P("ep", "tp", None),
        P(("ep", "tp"), None),
        P(("ep", "tp"), None),
    )
    return jax.shard_map(body, mesh=mesh, in_specs=placed, out_specs=P(("ep", "tp"), None), check_vma=False)
```

```python
import jax
import jax.numpy as jnp
from jax import lax
from jax.experimental import pallas as pl
from jax.experimental.pallas import tpu as pltpu
from jax.sharding import PartitionSpec as P

MESH = pl.DeviceIdType.MESH
CAP = 16
GROUPS = 8
PER = 64 // GROUPS
F32 = jnp.float32
BF16 = jnp.bfloat16
PLACES = (
    0o000, 0o121, 0o202, 0o323, 0o112, 0o233, 0o310, 0o031,
    0o220, 0o301, 0o022, 0o103, 0o332, 0o013, 0o130, 0o211,
    0o001, 0o122, 0o203, 0o320, 0o113, 0o230, 0o311, 0o032,
    0o221, 0o302, 0o023, 0o100, 0o333, 0o010, 0o131, 0o212,
    0o002, 0o123, 0o200, 0o321, 0o110, 0o231, 0o312, 0o033,
    0o222, 0o303, 0o020, 0o101, 0o330, 0o011, 0o132, 0o213,
    0o003, 0o120, 0o201, 0o322, 0o111, 0o232, 0o313, 0o030,
    0o223, 0o300, 0o021, 0o102, 0o331, 0o012, 0o133, 0o210,
)


def hops(i):
    digits = (PLACES[i] >> 6, (PLACES[i] >> 3) & 7, PLACES[i] & 7)
    return sum(min(d, 4 - d) for d in digits)


FARTHEST = sorted(range(1, 64), key=lambda i: -hops(i))


def kernel(
    tok, gain, bias, ids, rw, wg, wu, wd, out,
    rows_in, gain_in, bias_in, ids_in, rw_in,
    normed, spread, pick, send, recv, res, ret, vg, vu, vd, hid, whi, wlo, acc,
    in_sem, local_sem, wsend_sem, wrecv_sem, dsend, drecv, rsend, rrecv,
):
    ep, tp = lax.axis_index("ep"), lax.axis_index("tp")
    rows, width = tok.shape
    half = wg.shape[1]
    experts = lax.axis_size("ep")
    z, y, x = ep >> 4, (ep >> 2) & 3, ep & 3
    ahead = [[((at + d) & 3) << shift for d in range(4)] for at, shift in ((z, 4), (y, 2), (x, 0))]
    behind = [[((at - d) & 3) << shift for d in range(4)] for at, shift in ((z, 4), (y, 2), (x, 0))]

    def chip_at(i, steps):
        place = PLACES[i]
        return steps[0][place >> 6] | steps[1][(place >> 3) & 7] | steps[2][place & 7]

    block = rows // 4
    inputs = [
        pltpu.make_async_copy(a, b, in_sem.at[n])
        for n, (a, b) in enumerate(((ids, ids_in), (rw, rw_in), (gain, gain_in), (bias, bias_in)))
    ]
    token_rows = [
        pltpu.make_async_copy(tok.at[pl.ds(n * block, block)], rows_in.at[pl.ds(n * block, block)], in_sem.at[4 + n])
        for n in range(4)
    ]
    for copy in inputs + token_rows:
        copy.start()

    barrier = pltpu.get_barrier_semaphore()

    def greet(chip, core):
        pl.semaphore_signal(barrier, inc=1, device_id={"ep": chip, "tp": core}, device_id_type=MESH)

    for i in FARTHEST:
        greet(chip_at(i, ahead), tp)
    greet(ep, 1 - tp)

    mine = pl.ds(pl.multiple_of(tp * half, half), half)
    pairs = ((wg, vg.at[tp]), (wu, vu.at[tp]), (wd, vd.at[mine]))
    local = [pltpu.make_async_copy(a, b, local_sem.at[n]) for n, (a, b) in enumerate(pairs)]
    shared = [
        pltpu.make_async_remote_copy(
            src_ref=a, dst_ref=b, send_sem=wsend_sem.at[n], recv_sem=wrecv_sem.at[n],
            device_id={"ep": ep, "tp": 1 - tp}, device_id_type=MESH,
        )
        for n, (a, b) in enumerate(pairs)
    ]

    with jax.named_scope("s_route"):
        later = lax.broadcasted_iota(jnp.int32, (rows, rows), 0) < lax.broadcasted_iota(jnp.int32, (rows, rows), 1)
        later = jnp.where(later, 1.0, 0.0).astype(BF16)
        total = experts * CAP
        lanes = lax.broadcasted_iota(jnp.int32, (CAP, 128), 1)
        for i in range(experts):
            spread[i * CAP : (i + 1) * CAP, :] = jnp.where(lanes == chip_at(i, ahead), 1.0, 0.0).astype(BF16)
        for copy in inputs:
            copy.wait()
        expert_rows = lax.broadcasted_iota(jnp.int32, (128, rows), 0)
        first, second = ids_in[0:1, :] == expert_rows, ids_in[1:2, :] == expert_rows
        named = first | second
        count = jnp.dot(jnp.where(named, 1.0, 0.0).astype(BF16), later, preferred_element_type=F32)
        slot = jnp.where(named, count, -1.0)
        slot_of = jnp.dot(spread[...], slot.astype(BF16), preferred_element_type=F32)
        wanted = (lax.broadcasted_iota(jnp.int32, (total, rows), 0) & 15).astype(F32)
        pick[...] = jnp.where(slot_of == wanted, 1.0, 0.0).astype(BF16)

    with jax.named_scope("s_ln"):
        step = 32

        def norm(n, carry):
            at = pl.ds(pl.multiple_of(n * step, step), step)
            values = rows_in[at, :].astype(F32)
            centre = values - jnp.mean(values, axis=-1, keepdims=True)
            spread = jnp.mean(centre * centre, axis=-1, keepdims=True)
            normed[at, :] = (centre * lax.rsqrt(spread + 1e-05) * gain_in[...] + bias_in[...]).astype(BF16)
            return carry

        for copy in token_rows:
            copy.wait()
        lax.fori_loop(0, rows // step, norm, 0)

    def dispatch_copy(i):
        return pltpu.make_async_remote_copy(
            src_ref=send.at[i], dst_ref=recv.at[i], send_sem=dsend.at[i], recv_sem=drecv.at[i],
            device_id={"ep": chip_at(i, ahead), "tp": tp}, device_id_type=MESH,
        )

    def return_copy(i):
        return pltpu.make_async_remote_copy(
            src_ref=res.at[i], dst_ref=ret.at[i], send_sem=rsend.at[i], recv_sem=rrecv.at[i],
            device_id={"ep": chip_at(i, behind), "tp": tp}, device_id_type=MESH,
        )

    def members(k, action):
        for g in range(GROUPS):

            @pl.when(k == g)
            def _():
                for i in range(max(g * PER, 1), (g + 1) * PER):
                    action(i)

    def fill(k):
        chosen = pick[pl.ds(pl.multiple_of(k * PER * CAP, PER * CAP), PER * CAP), :]
        for c in range(0, width, 512):
            piece = jnp.dot(chosen, normed[:, c : c + 512], preferred_element_type=F32).astype(BF16)
            send[pl.ds(k * PER, PER), :, c : c + 512] = piece.reshape(PER, CAP, 512)

    fill(0)
    with jax.named_scope("s_bar"):
        pl.semaphore_wait(barrier, experts)
    for i in range(1, PER):
        dispatch_copy(i).start()
    for copy in shared:
        copy.start()
    for copy in local:
        copy.start()
    recv[0] = send[0]

    with jax.named_scope("s_push"):
        for k in range(1, GROUPS):
            fill(k)
            for i in range(k * PER, (k + 1) * PER):
                dispatch_copy(i).start()

    def to_rows(v):
        return lax.dot_general(v, spread[...], (((1,), (1,)), ((), ())), preferred_element_type=F32)

    weight = (jnp.where(first, rw_in[0:1, :], 0.0) + jnp.where(second, rw_in[1:2, :], 0.0)).T
    high = weight.astype(BF16)
    low = (weight - high.astype(F32)).astype(BF16)
    here = to_rows(slot.T.astype(BF16)) == (
        lax.broadcasted_iota(jnp.int32, (rows, total), 1) & 15
    ).astype(F32)
    whi[...] = jnp.where(here, to_rows(high), 0.0).astype(BF16)
    wlo[...] = jnp.where(here, to_rows(low), 0.0).astype(BF16)
    acc[...] = jnp.zeros_like(acc)

    with jax.named_scope("s_wwait"):
        for copy in local:
            copy.wait()
        for copy in shared:
            copy.wait_recv()

    def expert(k, carry):
        with jax.named_scope("s_dwait"):
            members(k, lambda i: dispatch_copy(i).wait_recv())
        x = recv[pl.ds(k * PER, PER)].reshape(PER * CAP, width)
        for t in range(2):
            for c in range(0, half, 256):
                gate = jnp.dot(x, vg[t, :, c : c + 256], preferred_element_type=F32)
                upper = jnp.dot(x, vu[t, :, c : c + 256], preferred_element_type=F32)
                hid[:, t * half + c : t * half + c + 256] = (gate / (1.0 + jnp.exp(-gate)) * upper).astype(BF16)
        for c in range(0, width, 256):
            piece = jnp.dot(hid[...], vd[:, c : c + 256], preferred_element_type=F32).astype(BF16)
            res[pl.ds(k * PER, PER), :, c : c + 256] = piece.reshape(PER, CAP, 256)
        with jax.named_scope("s_rsend"):
            members(k, lambda i: return_copy(i).start())
        return carry

    lax.fori_loop(0, GROUPS, expert, 0)
    ret[0] = res[0]

    for i in range(1, experts):
        dispatch_copy(i).wait_send()

    def part(k, c):
        at = pl.ds(pl.multiple_of(k * PER * CAP, PER * CAP), PER * CAP)
        y = ret[pl.ds(k * PER, PER), :, c : c + 512].reshape(PER * CAP, 512)
        return jnp.dot(whi[:, at], y, preferred_element_type=F32) + jnp.dot(wlo[:, at], y, preferred_element_type=F32)

    def combine(k, carry):
        with jax.named_scope("s_rwait"):
            members(k, lambda i: return_copy(i).wait_recv())
        for c in range(0, width, 512):
            acc[:, c : c + 512] += part(k, c)
        return carry

    lax.fori_loop(0, GROUPS - 1, combine, 0)
    with jax.named_scope("s_rlast"):
        for i in range((GROUPS - 1) * PER, GROUPS * PER):
            return_copy(i).wait_recv()
    with jax.named_scope("s_out"):
        for c in range(0, width, 512):
            out[:, c : c + 512] = (acc[:, c : c + 512] + part(GROUPS - 1, c)).astype(BF16)

    with jax.named_scope("s_end"):
        for copy in shared:
            copy.wait_send()
        for i in range(1, experts):
            return_copy(i).wait_send()


def body(tokens, norm_gain, norm_bias, gate_weight, up_weight, down_weight, expert_ids, route_weights):
    rows, width = tokens.shape
    half = gate_weight.shape[2]
    experts = lax.axis_size("ep")
    total = experts * CAP
    hbm = pl.BlockSpec(memory_space=pltpu.HBM)
    buffers = pltpu.VMEM((experts, CAP, width), BF16)
    copies = pltpu.SemaphoreType.DMA((experts,))
    three = pltpu.SemaphoreType.DMA((3,))
    return pl.pallas_call(
        kernel,
        name="experts",
        out_shape=jax.ShapeDtypeStruct((rows, width), BF16),
        in_specs=[hbm] * 8,
        out_specs=pl.BlockSpec(memory_space=pltpu.VMEM),
        scratch_shapes=[
            pltpu.VMEM((rows, width), BF16),
            pltpu.VMEM((1, width), F32),
            pltpu.VMEM((1, width), F32),
            pltpu.VMEM((2, rows), jnp.int32),
            pltpu.VMEM((2, rows), F32),
            pltpu.VMEM((rows, width), BF16),
            pltpu.VMEM((total, 128), BF16),
            pltpu.VMEM((total, rows), BF16),
            buffers, buffers, buffers, buffers,
            pltpu.VMEM((2, width, half), BF16),
            pltpu.VMEM((2, width, half), BF16),
            pltpu.VMEM((2 * half, width), BF16),
            pltpu.VMEM((PER * CAP, 2 * half), BF16),
            pltpu.VMEM((rows, total), BF16),
            pltpu.VMEM((rows, total), BF16),
            pltpu.VMEM((rows, width), F32),
            pltpu.SemaphoreType.DMA((8,)),
            three, three, three, copies, copies, copies, copies,
        ],
        compiler_params=pltpu.CompilerParams(
            collective_id=0, has_side_effects=True, vmem_limit_bytes=52 * 1024 * 1024
        ),
    )(*(
        pltpu.with_memory_space_constraint(array, pltpu.HBM)
        for array in (
            tokens, norm_gain.reshape(1, width), norm_bias.reshape(1, width), expert_ids.T, route_weights.T,
            gate_weight[0], up_weight[0], down_weight[0],
        )
    ))


def solution(mesh):
    placed = (
        P(("ep", "tp"), None),
        P(),
        P(),
        P("ep", None, "tp"),
        P("ep", None, "tp"),
        P("ep", "tp", None),
        P(("ep", "tp"), None),
        P(("ep", "tp"), None),
    )
    return jax.shard_map(body, mesh=mesh, in_specs=placed, out_specs=P(("ep", "tp"), None), check_vma=False)
```

```python
import jax
import jax.numpy as jnp
from jax import lax
from jax.experimental import pallas as pl
from jax.experimental.pallas import tpu as pltpu
from jax.sharding import PartitionSpec as P

MESH = pl.DeviceIdType.MESH
CAP = 16
GROUPS = 8
PER = 64 // GROUPS
F32 = jnp.float32
BF16 = jnp.bfloat16
PLACES = (
    0o000, 0o121, 0o202, 0o323, 0o112, 0o233, 0o310, 0o031,
    0o220, 0o301, 0o022, 0o103, 0o332, 0o013, 0o130, 0o211,
    0o001, 0o122, 0o203, 0o320, 0o113, 0o230, 0o311, 0o032,
    0o221, 0o302, 0o023, 0o100, 0o333, 0o010, 0o131, 0o212,
    0o002, 0o123, 0o200, 0o321, 0o110, 0o231, 0o312, 0o033,
    0o222, 0o303, 0o020, 0o101, 0o330, 0o011, 0o132, 0o213,
    0o003, 0o120, 0o201, 0o322, 0o111, 0o232, 0o313, 0o030,
    0o223, 0o300, 0o021, 0o102, 0o331, 0o012, 0o133, 0o210,
)


def hops(i):
    digits = (PLACES[i] >> 6, (PLACES[i] >> 3) & 7, PLACES[i] & 7)
    return sum(min(d, 4 - d) for d in digits)


FARTHEST = sorted(range(1, 64), key=lambda i: -hops(i))


def kernel(
    tok, gain, bias, ids, rw, wg, wu, wd, out,
    rows_in, gain_in, bias_in, ids_in, rw_in,
    normed, spread, pick, send, recv, res, ret, vg, vu, vd, hid, whi, wlo, wend, acc,
    in_sem, local_sem, wsend_sem, wrecv_sem, dsend, drecv, rsend, rrecv,
):
    ep, tp = lax.axis_index("ep"), lax.axis_index("tp")
    rows, width = tok.shape
    half = wg.shape[1]
    experts = lax.axis_size("ep")
    z, y, x = ep >> 4, (ep >> 2) & 3, ep & 3
    ahead = [[((at + d) & 3) << shift for d in range(4)] for at, shift in ((z, 4), (y, 2), (x, 0))]
    behind = [[((at - d) & 3) << shift for d in range(4)] for at, shift in ((z, 4), (y, 2), (x, 0))]

    def chip_at(i, steps):
        place = PLACES[i]
        return steps[0][place >> 6] | steps[1][(place >> 3) & 7] | steps[2][place & 7]

    block = rows // 4
    inputs = [
        pltpu.make_async_copy(a, b, in_sem.at[n])
        for n, (a, b) in enumerate(((ids, ids_in), (rw, rw_in), (gain, gain_in), (bias, bias_in)))
    ]
    token_rows = [
        pltpu.make_async_copy(tok.at[pl.ds(n * block, block)], rows_in.at[pl.ds(n * block, block)], in_sem.at[4 + n])
        for n in range(4)
    ]
    for copy in inputs + token_rows:
        copy.start()

    barrier = pltpu.get_barrier_semaphore()

    def greet(chip, core):
        pl.semaphore_signal(barrier, inc=1, device_id={"ep": chip, "tp": core}, device_id_type=MESH)

    for i in FARTHEST:
        greet(chip_at(i, ahead), tp)
    greet(ep, 1 - tp)

    mine = pl.ds(pl.multiple_of(tp * half, half), half)
    pairs = ((wg, vg.at[tp]), (wu, vu.at[tp]), (wd, vd.at[mine]))
    local = [pltpu.make_async_copy(a, b, local_sem.at[n]) for n, (a, b) in enumerate(pairs)]
    shared = [
        pltpu.make_async_remote_copy(
            src_ref=a, dst_ref=b, send_sem=wsend_sem.at[n], recv_sem=wrecv_sem.at[n],
            device_id={"ep": ep, "tp": 1 - tp}, device_id_type=MESH,
        )
        for n, (a, b) in enumerate(pairs)
    ]

    with jax.named_scope("s_route"):
        later = lax.broadcasted_iota(jnp.int32, (rows, rows), 0) < lax.broadcasted_iota(jnp.int32, (rows, rows), 1)
        later = jnp.where(later, 1.0, 0.0).astype(BF16)
        total = experts * CAP
        lanes = lax.broadcasted_iota(jnp.int32, (CAP, 128), 1)
        for i in range(experts):
            spread[i * CAP : (i + 1) * CAP, :] = jnp.where(lanes == chip_at(i, ahead), 1.0, 0.0).astype(BF16)
        for copy in inputs:
            copy.wait()
        expert_rows = lax.broadcasted_iota(jnp.int32, (128, rows), 0)
        first, second = ids_in[0:1, :] == expert_rows, ids_in[1:2, :] == expert_rows
        named = first | second
        count = jnp.dot(jnp.where(named, 1.0, 0.0).astype(BF16), later, preferred_element_type=F32)
        slot = jnp.where(named, count, -1.0)
        slot_of = jnp.dot(spread[...], slot.astype(BF16), preferred_element_type=F32)
        wanted = (lax.broadcasted_iota(jnp.int32, (total, rows), 0) & 15).astype(F32)
        pick[...] = jnp.where(slot_of == wanted, 1.0, 0.0).astype(BF16)

    with jax.named_scope("s_ln"):
        step = 32

        def norm(n, carry):
            at = pl.ds(pl.multiple_of(n * step, step), step)
            values = rows_in[at, :].astype(F32)
            centre = values - jnp.mean(values, axis=-1, keepdims=True)
            spread = jnp.mean(centre * centre, axis=-1, keepdims=True)
            normed[at, :] = (centre * lax.rsqrt(spread + 1e-05) * gain_in[...] + bias_in[...]).astype(BF16)
            return carry

        for copy in token_rows:
            copy.wait()
        lax.fori_loop(0, rows // step, norm, 0)

    def dispatch_copy(i):
        return pltpu.make_async_remote_copy(
            src_ref=send.at[i], dst_ref=recv.at[i], send_sem=dsend.at[i], recv_sem=drecv.at[i],
            device_id={"ep": chip_at(i, ahead), "tp": tp}, device_id_type=MESH,
        )

    def return_copy(i):
        return pltpu.make_async_remote_copy(
            src_ref=res.at[i], dst_ref=ret.at[i], send_sem=rsend.at[i], recv_sem=rrecv.at[i],
            device_id={"ep": chip_at(i, behind), "tp": tp}, device_id_type=MESH,
        )

    def members(k, action):
        for g in range(GROUPS):

            @pl.when(k == g)
            def _():
                for i in range(max(g * PER, 1), (g + 1) * PER):
                    action(i)

    def fill(k):
        chosen = pick[pl.ds(pl.multiple_of(k * PER * CAP, PER * CAP), PER * CAP), :]
        for c in range(0, width, 512):
            piece = jnp.dot(chosen, normed[:, c : c + 512], preferred_element_type=F32).astype(BF16)
            send[pl.ds(k * PER, PER), :, c : c + 512] = piece.reshape(PER, CAP, 512)

    fill(0)
    with jax.named_scope("s_bar"):
        pl.semaphore_wait(barrier, experts)
    for i in range(1, PER):
        dispatch_copy(i).start()
    for copy in local:
        copy.start()
    recv[0] = send[0]

    with jax.named_scope("s_push"):
        for k in range(1, GROUPS):
            fill(k)
            for i in range(k * PER, (k + 1) * PER):
                dispatch_copy(i).start()

    for copy in shared:
        copy.start()

    def to_rows(v):
        return lax.dot_general(v, spread[...], (((1,), (1,)), ((), ())), preferred_element_type=F32)

    weight = (jnp.where(first, rw_in[0:1, :], 0.0) + jnp.where(second, rw_in[1:2, :], 0.0)).T
    high = weight.astype(BF16)
    low = (weight - high.astype(F32)).astype(BF16)
    here = to_rows(slot.T.astype(BF16)) == (
        lax.broadcasted_iota(jnp.int32, (rows, total), 1) & 15
    ).astype(F32)
    whi[...] = jnp.where(here, to_rows(high), 0.0).astype(BF16)
    wlo[...] = jnp.where(here, to_rows(low), 0.0).astype(BF16)
    acc[...] = jnp.zeros_like(acc)
    tail = pl.ds(total - PER * CAP // 2, PER * CAP // 2)
    wend[...] = jnp.concatenate((whi[:, tail], wlo[:, tail]), axis=1)

    with jax.named_scope("s_wwait"):
        for copy in local:
            copy.wait()
        for copy in shared:
            copy.wait_recv()

    def expert(k, carry):
        with jax.named_scope("s_dwait"):
            members(k, lambda i: dispatch_copy(i).wait_recv())
        x = recv[pl.ds(k * PER, PER)].reshape(PER * CAP, width)
        for t in range(2):
            for c in range(0, half, 256):
                gate = jnp.dot(x, vg[t, :, c : c + 256], preferred_element_type=F32)
                upper = jnp.dot(x, vu[t, :, c : c + 256], preferred_element_type=F32)
                hid[:, t * half + c : t * half + c + 256] = (gate / (1.0 + jnp.exp(-gate)) * upper).astype(BF16)
        for c in range(0, width, 256):
            piece = jnp.dot(hid[...], vd[:, c : c + 256], preferred_element_type=F32).astype(BF16)
            res[pl.ds(k * PER, PER), :, c : c + 256] = piece.reshape(PER, CAP, 256)
        with jax.named_scope("s_rsend"):
            members(k, lambda i: return_copy(i).start())
        return carry

    lax.fori_loop(0, GROUPS, expert, 0)
    ret[0] = res[0]

    for i in range(1, experts):
        dispatch_copy(i).wait_send()

    def part(k, c):
        at = pl.ds(pl.multiple_of(k * PER * CAP, PER * CAP), PER * CAP)
        y = ret[pl.ds(k * PER, PER), :, c : c + 512].reshape(PER * CAP, 512)
        return jnp.dot(whi[:, at], y, preferred_element_type=F32) + jnp.dot(wlo[:, at], y, preferred_element_type=F32)

    def combine(k, carry):
        with jax.named_scope("s_rwait"):
            members(k, lambda i: return_copy(i).wait_recv())
        for c in range(0, width, 512):
            acc[:, c : c + 512] += part(k, c)
        return carry

    lax.fori_loop(0, GROUPS - 1, combine, 0)
    cut = experts - PER // 2
    for i in range((GROUPS - 1) * PER, cut):
        return_copy(i).wait_recv()
    rest = (experts - cut) * CAP
    for c in range(0, width, 512):
        y = ret[(GROUPS - 1) * PER : cut, :, c : c + 512].reshape(rest, 512)
        at = pl.ds(total - 2 * rest, rest)
        acc[:, c : c + 512] += jnp.dot(whi[:, at], y, preferred_element_type=F32) + jnp.dot(
            wlo[:, at], y, preferred_element_type=F32
        )
    with jax.named_scope("s_rlast"):
        for i in range(cut, experts):
            return_copy(i).wait_recv()
    with jax.named_scope("s_out"):
        for c in range(0, width, 512):
            y = ret[cut:experts, :, c : c + 512].reshape(rest, 512)
            y = jnp.dot(wend[...], jnp.concatenate((y, y), axis=0), preferred_element_type=F32)
            out[:, c : c + 512] = (acc[:, c : c + 512] + y).astype(BF16)

    with jax.named_scope("s_end"):
        for copy in shared:
            copy.wait_send()
        for i in range(1, experts):
            return_copy(i).wait_send()


def body(tokens, norm_gain, norm_bias, gate_weight, up_weight, down_weight, expert_ids, route_weights):
    rows, width = tokens.shape
    half = gate_weight.shape[2]
    experts = lax.axis_size("ep")
    total = experts * CAP
    hbm = pl.BlockSpec(memory_space=pltpu.HBM)
    buffers = pltpu.VMEM((experts, CAP, width), BF16)
    copies = pltpu.SemaphoreType.DMA((experts,))
    three = pltpu.SemaphoreType.DMA((3,))
    return pl.pallas_call(
        kernel,
        name="experts",
        out_shape=jax.ShapeDtypeStruct((rows, width), BF16),
        in_specs=[hbm] * 8,
        out_specs=pl.BlockSpec(memory_space=pltpu.VMEM),
        scratch_shapes=[
            pltpu.VMEM((rows, width), BF16),
            pltpu.VMEM((1, width), F32),
            pltpu.VMEM((1, width), F32),
            pltpu.VMEM((2, rows), jnp.int32),
            pltpu.VMEM((2, rows), F32),
            pltpu.VMEM((rows, width), BF16),
            pltpu.VMEM((total, 128), BF16),
            pltpu.VMEM((total, rows), BF16),
            buffers, buffers, buffers, buffers,
            pltpu.VMEM((2, width, half), BF16),
            pltpu.VMEM((2, width, half), BF16),
            pltpu.VMEM((2 * half, width), BF16),
            pltpu.VMEM((PER * CAP, 2 * half), BF16),
            pltpu.VMEM((rows, total), BF16),
            pltpu.VMEM((rows, total), BF16),
            pltpu.VMEM((rows, PER * CAP), BF16),
            pltpu.VMEM((rows, width), F32),
            pltpu.SemaphoreType.DMA((8,)),
            three, three, three, copies, copies, copies, copies,
        ],
        compiler_params=pltpu.CompilerParams(
            collective_id=0, has_side_effects=True, vmem_limit_bytes=52 * 1024 * 1024
        ),
    )(*(
        pltpu.with_memory_space_constraint(array, pltpu.HBM)
        for array in (
            tokens, norm_gain.reshape(1, width), norm_bias.reshape(1, width), expert_ids.T, route_weights.T,
            gate_weight[0], up_weight[0], down_weight[0],
        )
    ))


def solution(mesh):
    placed = (
        P(("ep", "tp"), None),
        P(),
        P(),
        P("ep", None, "tp"),
        P("ep", None, "tp"),
        P("ep", "tp", None),
        P(("ep", "tp"), None),
        P(("ep", "tp"), None),
    )
    return jax.shard_map(body, mesh=mesh, in_specs=placed, out_specs=P(("ep", "tp"), None), check_vma=False)
```
